128 devices in a mesh: ep: 128 (over z, y, x, core).
Axes of the slice: x: 4, y: 4, z: 4, core: 2. Of those that a mesh axis runs over, the one named last changes fastest.
Arguments:
- residual_in: bfloat16 [1024, 2048], P('ep'), may hold values from -6 to 6
- gain_mix_pre: float32 [2048], replicated, may hold values from 0.1 to 1.9
- w_query: bfloat16 [2048, 2048], P(None, 'ep'), may hold values from -0.125 to 0.125
- w_key: bfloat16 [2048, 2048], P(None, 'ep'), may hold values from -0.125 to 0.125
- w_value: bfloat16 [2048, 2048], P(None, 'ep'), may hold values from -0.125 to 0.125
- w_outgate: bfloat16 [2048, 2048], P(None, 'ep'), may hold values from -0.125 to 0.125
- w_decay: bfloat16 [2048, 16], replicated, may hold values from -0.125 to 0.125
- w_beta: bfloat16 [2048, 16], replicated, may hold values from -0.125 to 0.125
- decay_scale: float32 [16], replicated, may hold values from 1 to 16
- decay_bias: float32 [16], replicated, may hold values from -5 to -1
- head_gain: float32 [128], replicated, may hold values from 0.1 to 1.9
- w_out: bfloat16 [2048, 2048], replicated, may hold values from -0.125 to 0.125
- gain_mix_post: float32 [2048], replicated, may hold values from 0.1 to 1.9
- state_cache: bfloat16 [1024, 16, 128, 128], P('ep'), may hold values from -2.390625 to 2.390625
- gain_ffn_pre: float32 [2048], replicated, may hold values from 0.1 to 1.9
- routes: int32 [1024, 4], P('ep'), may hold values from 0 to 31, all different within a row; in each aligned block of 8 rows (0 to 7, 8 to 15, ...) at most 2 rows name the same one
- route_logits: float32 [1024, 4], P('ep'), may hold values from -6 to 6
- w_gate: bfloat16 [2048, 65536], P(None, 'ep'), may hold values from -0.375 to 0.375
- w_up: bfloat16 [2048, 65536], P(None, 'ep'), may hold values from -0.375 to 0.375
- w_down: bfloat16 [65536, 2048], P('ep'), may hold values from -0.125 to 0.125
- gain_ffn_post: float32 [2048], replicated, may hold values from 0.1 to 1.9
Outputs:
- result: bfloat16 [1024, 2048], P('ep')
- new_state: bfloat16 [1024, 16, 128, 128], P('ep')
The draws below stay inside these ranges and needn't reach their ends.
Inputs may be any that keep to these rules, and one draw needn't show every extreme that they name: `routes`: each row names 4 different experts. In the rows of one device (aligned blocks of 8 rows) no expert is named more than 2 times, and in some block one expert is named exactly 2 times.
All inputs are finite; a program needn't handle non-finite values.
Results may differ from the reference program's by a relative error of at most 0.014.
Values may be sent and summed in bfloat16 or wider, within the bound.
No kernel may reach another device: no remote copies, remote signals or barrier semaphores. Data moves between devices by JAX's collectives and lax.ppermute only.
A program may use at most 128 MiB of HBM per device.

```python
import math
import jax
import jax.numpy as jnp
import numpy as np
from jax import lax

D = 2048
H = 16
HD = 128
FF = 2048
PIECES = 4
TOPK = 4
SEQ_DEV = 8
TOKENS = 1024
EXPERTS = 32
CAP = 2
N_EP = 128


def level_of(own_key, shape, shards, low, top_value):
    def one(position, blocks):
        steps = jax.random.uniform(jax.random.fold_in(jax.random.fold_in(own_key, 6), position), (blocks,), jnp.float32, low / len(shards), top_value / len(shards))
        return jnp.repeat(jnp.exp(steps), shape[position] // blocks).reshape((-1,) + (1,) * (len(shape) - position - 1))

    gain = one(*shards[0])
    for cut in shards[1:]:
        gain = gain * one(*cut)
    return gain


def deal_out(stream_key, own, number, rows, count, top, limit, lean):
    ranking = jax.random.permutation(stream_key, count)
    heavy_load, common = shares(count, rows * top, limit, lean, True), shares(count, rows * top, limit, lean, False)
    places = jnp.arange(count)

    def named(sizes, rotation):
        used = int((sizes > 0).sum())
        fixed = max(1, used // 4)
        moved = fixed + (places - fixed + rotation * (used - fixed)) % max(1, count - fixed)
        return jnp.zeros((count,), jnp.int32).at[ranking[jnp.where(places < fixed, places, moved)]].set(jnp.asarray(sizes, jnp.int32))

    sizes = jnp.where(number % 4 == 0, named(heavy_load, number // 4), named(common, number - number // 4 - 1))
    mixed = jax.random.permutation(jax.random.fold_in(own, 3), count)
    source_of, receiver = mixed[0:count // 2 * 2:2], mixed[1:count // 2 * 2:2]
    room = jnp.minimum(sizes[source_of] - 1, limit - sizes[receiver]) // 2
    room = jnp.where((source_of == ranking[0]) | (receiver == ranking[0]) | (sizes[receiver] == 0), 0, jnp.maximum(room, 0))
    moved = jax.random.randint(jax.random.fold_in(own, 4), (count // 2,), 0, 1 << 20) % (room + 1)
    sizes = sizes.at[source_of].add(-moved).at[receiver].add(moved)
    members = jnp.searchsorted(jnp.cumsum(sizes), jnp.arange(rows * top), side="right").astype(jnp.int32)
    table = members.reshape(top, rows).T
    table = table[jax.random.permutation(jax.random.fold_in(own, 1), rows)]
    rotation = jax.random.randint(jax.random.fold_in(own, 2), (rows, 1), 0, top)
    return jnp.take_along_axis(table, (jnp.arange(top)[None, :] + rotation) % top, axis=1)


def shares(number_of, total, bound, slope, full):
    loads = [(1 << 20) // math.isqrt(standing ** slope) + 1 for standing in range(1, number_of + 1)]
    largest = bound if full else min(bound, max(-(-total // number_of), total * loads[0] // sum(loads)))
    least = 1 if total - largest >= number_of - 1 else 0
    holding, rest = [largest] + [least] * (number_of - 1), total - largest - least * (number_of - 1)
    while rest > 0:
        free = [i for i in range(1, number_of) if holding[i] < largest] or [i for i in range(1, number_of) if holding[i] < bound]
        mass, remaining = sum([loads[i] for i in free]), rest
        for i in free:
            more = min(bound - holding[i], max(1, remaining * loads[i] // mass), rest)
            holding[i] = holding[i] + more
            rest = rest - more
    return np.array(holding)


def noise(key, shape, scale, limit, pieces=(), held_as=jnp.bfloat16):
    values = scale * jax.random.normal(key, shape, jnp.float32)
    if pieces:
        values = values * level_of(key, shape, pieces, -0.22, 0.18)
    return jnp.clip(values, -limit, limit).astype(held_as)


def setup_inputs(seed: int = 0) -> dict:
    key_of = jax.random.split(jax.random.key(seed), 22)
    residual_in = noise(key_of[0], (TOKENS, D), 1.0, 6.0, ((0, 128),))
    gain_mix_pre = jnp.clip(1.0 + 0.18 * jax.random.normal(key_of[1], (D,), jnp.float32), 0.1, 1.9)
    w_query = noise(key_of[2], (D, H * HD), D ** -0.5, 0.125, ((1, 128),))
    w_key = noise(key_of[3], (D, H * HD), D ** -0.5, 0.125, ((1, 128),))
    w_value = noise(key_of[4], (D, H * HD), D ** -0.5, 0.125, ((1, 128),))
    w_outgate = noise(key_of[5], (D, H * HD), D ** -0.5, 0.125, ((1, 128),))
    w_decay = noise(key_of[6], (D, H), D ** -0.5, 0.125)
    w_beta = noise(key_of[7], (D, H), D ** -0.5, 0.125)
    decay_scale = jnp.clip(jnp.exp(jax.random.uniform(key_of[8], (H,), jnp.float32, math.log(1.0), math.log(16.0))), 1.0, 16.0)
    decay_bias = jnp.clip(jax.random.uniform(key_of[9], (H,), jnp.float32, -5.0, -1.0), -5.0, -1.0)
    head_gain = jnp.clip(1.0 + 0.18 * jax.random.normal(key_of[10], (HD,), jnp.float32), 0.1, 1.9)
    w_out = noise(key_of[11], (H * HD, D), (H * HD) ** -0.5, 0.125)
    gain_mix_post = jnp.clip(1.0 + 0.18 * jax.random.normal(key_of[12], (D,), jnp.float32), 0.1, 1.9)
    state_cache = noise(key_of[13], (TOKENS, H, HD, HD), 0.3, 2.390625, ((0, 128),))
    gain_ffn_pre = jnp.clip(1.0 + 0.18 * jax.random.normal(key_of[14], (D,), jnp.float32), 0.1, 1.9)
    routes_keys = jax.random.split(jax.random.fold_in(key_of[15], 1), TOKENS // SEQ_DEV)
    routes_turns = jax.random.permutation(jax.random.fold_in(key_of[15], 3), TOKENS // SEQ_DEV)
    routes = jax.vmap(lambda own, number: deal_out(jax.random.fold_in(key_of[15], 2), own, number, SEQ_DEV, EXPERTS, TOPK, CAP, 1))(routes_keys, routes_turns).reshape((TOKENS, TOPK))
    route_logits = noise(key_of[16], (TOKENS, TOPK), 1.0, 6.0, ((0, 128),), jnp.float32)
    w_gate = noise(key_of[17], (D, EXPERTS * FF), (D // 9) ** -0.5, 0.375, ((1, 128),))
    w_up = noise(key_of[18], (D, EXPERTS * FF), (D // 9) ** -0.5, 0.375, ((1, 128),))
    w_down = noise(key_of[19], (EXPERTS * FF, D), FF ** -0.5, 0.125, ((0, 128),))
    gain_ffn_post = jnp.clip(1.0 + 0.18 * jax.random.normal(key_of[20], (D,), jnp.float32), 0.1, 1.9)
    return dict(residual_in=residual_in, gain_mix_pre=gain_mix_pre, w_query=w_query, w_key=w_key, w_value=w_value, w_outgate=w_outgate, w_decay=w_decay, w_beta=w_beta, decay_scale=decay_scale, decay_bias=decay_bias, head_gain=head_gain, w_out=w_out, gain_mix_post=gain_mix_post, state_cache=state_cache, gain_ffn_pre=gain_ffn_pre, routes=routes, route_logits=route_logits, w_gate=w_gate, w_up=w_up, w_down=w_down, gain_ffn_post=gain_ffn_post)


EPS = 1e-06
LIMIT = 7.0
ALPHA = 1.702

def rms_scale(values):
    return values * lax.rsqrt(lax.optimization_barrier(jnp.mean(values * values, axis=-1, keepdims=True)) + EPS)

def clamped_unit(gate, upper):
    glu = jnp.minimum(gate, LIMIT)
    linear = jnp.clip(upper, -LIMIT, LIMIT)
    return glu * jax.nn.sigmoid(ALPHA * glu) * (linear + 1.0)

def dispatch_table(routes, experts, capacity):
    count, topk = routes.shape
    hits = (routes[:, :, None] == jnp.arange(experts, dtype=jnp.int32)).astype(jnp.int32)
    flat = hits.reshape(count * topk, experts)
    before = jnp.cumsum(flat, axis=0) - flat
    slots = lax.optimization_barrier(jnp.sum(before * flat, axis=1)).reshape(count, topk)
    target = routes * capacity + slots
    return (target[:, :, None] == jnp.arange(experts * capacity, dtype=jnp.int32)).astype(jnp.float32)

def delta_step(q_raw, k_raw, v_raw, z_raw, decay_in, beta_in, state, decay_scale, decay_bias, head_gain):
    count = q_raw.shape[0]
    query = jax.nn.silu(q_raw.astype(jnp.float32)).reshape(count, H, HD)
    query = query * lax.rsqrt(lax.optimization_barrier(jnp.sum(query * query, axis=-1, keepdims=True)) + EPS) * HD ** (-0.5)
    keys = jax.nn.silu(k_raw.astype(jnp.float32)).reshape(count, H, HD)
    keys = keys * lax.rsqrt(lax.optimization_barrier(jnp.sum(keys * keys, axis=-1, keepdims=True)) + EPS)
    values = jax.nn.silu(v_raw.astype(jnp.float32)).reshape(count, H, HD)
    decay = -decay_scale * jax.nn.softplus(decay_in + decay_bias)
    beta = jax.nn.sigmoid(beta_in)
    held = state.astype(jnp.float32) * jnp.exp(decay)[:, :, None, None]
    guess = jnp.einsum('rhk,rhkv->rhv', keys, held)
    held = held + jnp.einsum('rhk,rhv->rhkv', keys, beta[:, :, None] * (values - guess))
    output = jnp.einsum('rhk,rhkv->rhv', query, held)
    output = rms_scale(output) * head_gain
    gated = output.reshape(count, H * HD) * jax.nn.silu(z_raw.astype(jnp.float32))
    return (gated.astype(jnp.bfloat16), held.astype(jnp.bfloat16))

def reference(residual_in, gain_mix_pre, w_query, w_key, w_value, w_outgate, w_decay, w_beta, decay_scale, decay_bias, head_gain, w_out, gain_mix_post, state_cache, gain_ffn_pre, routes, route_logits, w_gate, w_up, w_down, gain_ffn_post):
    x_first = residual_in.astype(jnp.float32)
    normed = (rms_scale(x_first) * gain_mix_pre).astype(jnp.bfloat16)

    def project(weight):
        return jnp.dot(normed, weight, preferred_element_type=jnp.float32).astype(jnp.bfloat16)
    q_raw, k_raw, v_raw, z_raw = (project(w_query), project(w_key), project(w_value), project(w_outgate))
    decay_in = jnp.dot(normed, w_decay, preferred_element_type=jnp.float32)
    beta_in = jnp.dot(normed, w_beta, preferred_element_type=jnp.float32)

    def blocks(array):
        return array.reshape((N_EP, SEQ_DEV) + array.shape[1:])

    def block_step(items):
        return delta_step(*items, decay_scale, decay_bias, head_gain)
    mixed, new_state = lax.map(block_step, tuple((blocks(a) for a in (q_raw, k_raw, v_raw, z_raw, decay_in, beta_in, state_cache))))
    mixed = mixed.reshape(TOKENS, H * HD)
    new_state = new_state.reshape(TOKENS, H, HD, HD)
    branch = jnp.dot(mixed, w_out, preferred_element_type=jnp.float32)
    x_second = x_first + rms_scale(branch) * gain_mix_post
    normed_two = (rms_scale(x_second) * gain_ffn_pre).astype(jnp.bfloat16)
    table = jax.vmap(lambda r: dispatch_table(r, EXPERTS, CAP))(routes.reshape(N_EP, SEQ_DEV, TOPK))
    picks = lax.optimization_barrier(jnp.sum(table, axis=2))
    sent = jnp.einsum('nse,nsd->ned', picks, normed_two.reshape(N_EP, SEQ_DEV, D).astype(jnp.float32), precision=lax.Precision.HIGHEST).astype(jnp.bfloat16)
    sent = sent.reshape(N_EP, EXPERTS, CAP, D).transpose(1, 0, 2, 3).reshape(EXPERTS, N_EP * CAP, D)
    width = FF // PIECES

    def expert(items):
        rows_in, index = items
        total = jnp.zeros((N_EP * CAP, D), jnp.float32)
        for part in range(PIECES):
            start = (index * FF + part * width).astype(jnp.int32)
            gate_cols = lax.dynamic_slice_in_dim(w_gate, start, width, 1)
            up_cols = lax.dynamic_slice_in_dim(w_up, start, width, 1)
            down_rows = lax.dynamic_slice_in_dim(w_down, start, width, 0)
            hidden = clamped_unit(jnp.dot(rows_in, gate_cols, preferred_element_type=jnp.float32), jnp.dot(rows_in, up_cols, preferred_element_type=jnp.float32)).astype(jnp.bfloat16)
            piece_out = jnp.dot(hidden, down_rows, preferred_element_type=jnp.float32).astype(jnp.bfloat16)
            piece_out = lax.optimization_barrier(piece_out)
            total = total + piece_out.astype(jnp.float32)
        return total
    outputs = lax.map(expert, (sent, jnp.arange(EXPERTS, dtype=jnp.int32)))
    outputs = outputs.reshape(EXPERTS, N_EP, CAP, D).transpose(1, 0, 2, 3).reshape(N_EP, EXPERTS * CAP, D)
    raised = jnp.exp(route_logits)
    weights = raised / lax.optimization_barrier(jnp.sum(raised, axis=-1, keepdims=True))
    mix_table = jnp.einsum('nske,nsk->nse', table, weights.reshape(N_EP, SEQ_DEV, TOPK))
    moe = jnp.einsum('nse,ned->nsd', mix_table, outputs, precision=lax.Precision.HIGHEST).reshape(TOKENS, D)
    result = (x_second + rms_scale(moe) * gain_ffn_post).astype(jnp.bfloat16)
    return (result, new_state)
```

```python
import jax
import jax.numpy as jnp
from jax import lax
from jax.sharding import Mesh
from jax.sharding import PartitionSpec as P

H = 16
HD = 128
TOPK = 4
EXPERTS = 32
CAP = 2
ZY = 16
CHIPS = 64
QUART = 4


EPS = 1e-06
LIMIT = 7.0
ALPHA = 1.702


def rms_scale(values):
    return values * lax.rsqrt(jnp.mean(values * values, axis=-1, keepdims=True) + EPS)


def clamped_unit(gate, upper):
    glu = jnp.minimum(gate, LIMIT)
    linear = jnp.clip(upper, -LIMIT, LIMIT)
    return glu * jax.nn.sigmoid(ALPHA * glu) * (linear + 1.0)


def dispatch_table(routes, experts, capacity):
    count, topk = routes.shape
    hits = (routes[:, :, None] == jnp.arange(experts, dtype=jnp.int32)).astype(jnp.int32)
    flat = hits.reshape(count * topk, experts)
    before = jnp.cumsum(flat, axis=0) - flat
    slots = jnp.sum(before * flat, axis=1).reshape(count, topk)
    target = routes * capacity + slots
    return (target[:, :, None] == jnp.arange(experts * capacity, dtype=jnp.int32)).astype(
        jnp.float32
    )


def delta_step(
    q_raw, k_raw, v_raw, z_raw, decay_in, beta_in, state, decay_scale, decay_bias, head_gain
):
    count = q_raw.shape[0]
    query = jax.nn.silu(q_raw.astype(jnp.float32)).reshape(count, H, HD)
    query = query * lax.rsqrt(jnp.sum(query * query, axis=-1, keepdims=True) + EPS) * HD ** (-0.5)
    keys = jax.nn.silu(k_raw.astype(jnp.float32)).reshape(count, H, HD)
    keys = keys * lax.rsqrt(jnp.sum(keys * keys, axis=-1, keepdims=True) + EPS)
    values = jax.nn.silu(v_raw.astype(jnp.float32)).reshape(count, H, HD)
    decay = -decay_scale * jax.nn.softplus(decay_in + decay_bias)
    beta = jax.nn.sigmoid(beta_in)
    held = state.astype(jnp.float32) * jnp.exp(decay)[:, :, None, None]
    guess = jnp.einsum("rhk,rhkv->rhv", keys, held)
    held = held + jnp.einsum("rhk,rhv->rhkv", keys, beta[:, :, None] * (values - guess))
    output = jnp.einsum("rhk,rhkv->rhv", query, held)
    output = rms_scale(output) * head_gain
    gated = output.reshape(count, H * HD) * jax.nn.silu(z_raw.astype(jnp.float32))
    return (gated.astype(jnp.bfloat16), held.astype(jnp.bfloat16))


def swap_cores(values):
    return lax.ppermute(values, "c", [(0, 1), (1, 0)])


def shards(
    residual_in,
    gain_mix_pre,
    w_query,
    w_key,
    w_value,
    w_outgate,
    w_decay,
    w_beta,
    decay_scale,
    decay_bias,
    head_gain,
    w_out,
    gain_mix_post,
    state_cache,
    gain_ffn_pre,
    routes,
    route_logits,
    w_gate,
    w_up,
    w_down,
    gain_ffn_post,
):
    count, width = residual_in.shape
    x_at = lax.axis_index("x")
    c_at = lax.axis_index("c")
    rows = lax.all_to_all(
        jnp.broadcast_to(residual_in, (ZY, count, width)), ("z", "y"), 0, 0, tiled=True
    )
    own = jnp.concatenate([w_query.T, w_key.T, w_value.T, w_outgate.T], axis=0)
    mine = [own] + [
        lax.ppermute(own, "x", [(i, (i + shift) % 4) for i in range(4)]) for shift in (1, 2, 3)
    ]
    mine = jnp.stack(mine)
    other = swap_cores(mine)
    order = (x_at - jnp.arange(4)) % 4
    both = jnp.stack([mine[order], other[order]], axis=1)
    both = jnp.where(c_at == 0, both, both[:, ::-1])
    head_weights = both.reshape(4, 2, 4, 16, width).transpose(2, 0, 1, 3, 4).reshape(4 * HD, width)

    gate_other = swap_cores(w_gate)
    up_other = swap_cores(w_up)
    down_other = swap_cores(w_down)

    rows_first = rows.reshape(ZY * count, width).astype(jnp.float32)
    rows_normed = (rms_scale(rows_first) * gain_mix_pre).astype(jnp.bfloat16)
    columns = lax.dot_general(
        rows_normed, head_weights, (((1,), (1,)), ((), ())), preferred_element_type=jnp.float32
    ).astype(jnp.bfloat16)
    joined = lax.all_to_all(
        columns.reshape(ZY, count, 4 * HD), ("z", "y"), 0, 0, tiled=True
    )
    joined = joined.reshape(ZY, count, 4, HD).transpose(2, 1, 0, 3).reshape(4, count, H * HD)

    x_first = residual_in.astype(jnp.float32)
    normed = (rms_scale(x_first) * gain_mix_pre).astype(jnp.bfloat16)
    decay_in = jnp.dot(normed, w_decay, preferred_element_type=jnp.float32)
    beta_in = jnp.dot(normed, w_beta, preferred_element_type=jnp.float32)
    mixed, new_state = delta_step(
        joined[0],
        joined[1],
        joined[2],
        joined[3],
        decay_in,
        beta_in,
        state_cache,
        decay_scale,
        decay_bias,
        head_gain,
    )
    branch = jnp.dot(mixed, w_out, preferred_element_type=jnp.float32)
    x_second = x_first + rms_scale(branch) * gain_mix_post
    normed_two = (rms_scale(x_second) * gain_ffn_pre).astype(jnp.bfloat16)
    table = dispatch_table(routes, EXPERTS, CAP)
    picks = jnp.sum(table, axis=1)
    run = width // QUART
    placed = jnp.broadcast_to(
        picks.reshape(count, EXPERTS, 1, CAP), (count, EXPERTS, 2, CAP)
    ).reshape(count, CHIPS * CAP)
    choose = (
        placed.T[:, None, :, None] * jnp.eye(QUART, dtype=jnp.float32)[None, :, None, :]
    ).reshape(CHIPS * CAP * QUART, count * QUART)
    sent = jnp.dot(
        choose.astype(jnp.bfloat16),
        normed_two.reshape(count * QUART, run),
        preferred_element_type=jnp.float32,
    ).astype(jnp.bfloat16)
    block = lax.all_to_all(
        sent.reshape(CHIPS, CAP * QUART, run), ("z", "y", "x"), 0, 0, tiled=True
    )
    flat = block.reshape(CHIPS * CAP, width)

    def hidden_of(gate, upper):
        return clamped_unit(
            jnp.dot(flat, gate, preferred_element_type=jnp.float32),
            jnp.dot(flat, upper, preferred_element_type=jnp.float32),
        ).astype(jnp.bfloat16)

    partial_value = (
        jnp.dot(hidden_of(w_gate, w_up), w_down, preferred_element_type=jnp.float32)
        + jnp.dot(hidden_of(gate_other, up_other), down_other, preferred_element_type=jnp.float32)
    ).astype(jnp.bfloat16)
    returned = lax.all_to_all(
        partial_value.reshape(CHIPS, CAP * QUART, run), ("z", "y", "x"), 0, 0, tiled=True
    )
    summed = jnp.sum(returned.reshape(EXPERTS, 2, CAP, width).astype(jnp.float32), axis=1)
    summed = summed.reshape(EXPERTS * CAP, width)
    raised = jnp.exp(route_logits)
    weights = raised / jnp.sum(raised, axis=-1, keepdims=True)
    mix_table = jnp.einsum("ske,sk->se", table, weights)
    moe = jnp.dot(mix_table, summed)
    result = (x_second + rms_scale(moe) * gain_ffn_post).astype(jnp.bfloat16)
    return (result, new_state)


def solution(mesh):
    torus = Mesh(mesh.devices.reshape(4, 4, 4, 2), ("z", "y", "x", "c"))
    ep = ("z", "y", "x", "c")
    in_specs = (
        P(ep, None),
        P(),
        P(None, ep),
        P(None, ep),
        P(None, ep),
        P(None, ep),
        P(),
        P(),
        P(),
        P(),
        P(),
        P(),
        P(),
        P(ep, None, None, None),
        P(),
        P(ep, None),
        P(ep, None),
        P(None, ep),
        P(None, ep),
        P(ep, None),
        P(),
    )
    out_specs = (P(ep, None), P(ep, None, None, None))
    return jax.shard_map(
        shards, mesh=torus, in_specs=in_specs, out_specs=out_specs, check_vma=False
    )
```

```python
import jax
import jax.numpy as jnp
from jax import lax
from jax.experimental import pallas as pl
from jax.experimental.pallas import tpu as pltpu
from jax.sharding import Mesh
from jax.sharding import PartitionSpec as P


H = 16
HD = 128
D = 2048
TOPK = 4
EXPERTS = 32
CAP = 2
SEQ = 8
ZY = 16
CHIPS = 64
QUART = 4
RUN = D // QUART
LINES = CHIPS * CAP * QUART
ROWS = CHIPS * CAP


EPS = 1e-06
LIMIT = 7.0
ALPHA = 1.702

F32 = jnp.float32
BF16 = jnp.bfloat16
MIB = 1 << 20


def iota(shape, dimension):
    return lax.broadcasted_iota(jnp.int32, shape, dimension)


def nt(left, right):
    return lax.dot_general(left, right, (((1,), (1,)), ((), ())), preferred_element_type=F32)


def mm(left, right):
    return jnp.dot(left, right, preferred_element_type=F32)


def silu(values):
    return values * jax.nn.sigmoid(values)


def rms_scale(values):
    return values * lax.rsqrt(jnp.mean(values * values, axis=-1, keepdims=True) + EPS)


def halves(values):
    high = values.astype(BF16)
    return high, (values - high.astype(F32)).astype(BF16)


def clamped_unit(gate, upper):
    glu = jnp.minimum(gate, LIMIT)
    linear = jnp.clip(upper, -LIMIT, LIMIT)
    return glu * jax.nn.sigmoid(ALPHA * glu) * (linear + 1.0)


def call(body, outs, limit, scratch=(), specs=None, outs_specs=None, flops=0):
    return pl.pallas_call(
        body,
        out_shape=outs,
        **({} if specs is None else {"in_specs": specs}),
        **({} if outs_specs is None else {"out_specs": outs_specs}),
        scratch_shapes=list(scratch),
        compiler_params=pltpu.CompilerParams(vmem_limit_bytes=limit * MIB),
        cost_estimate=pl.CostEstimate(flops=flops, bytes_accessed=0, transcendentals=0),
    )


def shape(dims, dtype):
    return jax.ShapeDtypeStruct(dims, dtype)


def route_body(
    routes_ref,
    logits_ref,
    x_ref,
    gain_pre_ref,
    decay_w_ref,
    beta_w_ref,
    scale_ref,
    bias_ref,
    send_ref,
    mix_ref,
    fade_ref,
    beta_ref,
):
    normed = (rms_scale(x_ref[...].astype(F32)) * gain_pre_ref[...]).astype(BF16)
    raised = nt(normed, decay_w_ref[...]) + bias_ref[...]
    soft = jnp.maximum(raised, 0.0) + jnp.log1p(jnp.exp(-jnp.abs(raised)))
    fade_ref[...] = jnp.exp(-scale_ref[...] * soft)
    beta_ref[...] = jax.nn.sigmoid(nt(normed, beta_w_ref[...]))
    routes = routes_ref[...]
    raised = jnp.exp(logits_ref[...])
    weights = raised / jnp.sum(raised, axis=-1, keepdims=True)
    named = iota((SEQ, EXPERTS), 1)
    hits = jnp.zeros((SEQ, EXPERTS), F32)
    weighed = jnp.zeros((SEQ, EXPERTS), F32)
    for j in range(TOPK):
        hit = (routes[:, j : j + 1] == named).astype(F32)
        hits = hits + hit
        weighed = weighed + hit * weights[:, j : j + 1]
    earlier = (iota((SEQ, SEQ), 0) > iota((SEQ, SEQ), 1)).astype(BF16)
    slots = mm(earlier, hits.astype(BF16))
    line = iota((LINES, EXPERTS), 0)
    expert_of = (line // (2 * CAP * QUART)) == iota((LINES, EXPERTS), 1)
    slot_of = (line // QUART) % CAP
    column = iota((LINES, QUART * SEQ), 1)
    same_run = (iota((LINES, QUART * SEQ), 0) % QUART) == (column // SEQ)
    send = jnp.zeros((LINES, QUART * SEQ), F32)
    mix = jnp.zeros((LINES, QUART * SEQ), F32)
    for slot in range(CAP):
        chosen = (expert_of & (slot_of == slot)).astype(BF16)
        here = slots == slot
        picks = jnp.where(here, hits, 0.0)
        shares = jnp.where(here, weighed, 0.0)
        high, low = halves(jnp.concatenate([shares] * QUART, axis=0))
        send = send + nt(chosen, jnp.concatenate([picks] * QUART, axis=0).astype(BF16))
        mix = mix + (nt(chosen, high) + nt(chosen, low))
    send_ref[...] = jnp.where(same_run, send, 0.0).astype(BF16)
    high, low = halves(jnp.where(same_run, mix, 0.0).T)
    mix_ref[...] = jnp.concatenate([high, low], axis=0)


def prepare_body(x_ref, q_ref, k_ref, v_ref, z_ref, rows_ref, own_ref, near_ref, wide_ref, sems):
    fetch = pltpu.make_async_copy(x_ref, near_ref, sems.at[4])
    fetch.start()
    copies = [
        pltpu.make_async_copy(ref, own_ref.at[pl.ds(i * 16, 16)], sems.at[i])
        for i, ref in enumerate((q_ref, k_ref, v_ref, z_ref))
    ]
    for copy in copies:
        copy.start()
    fetch.wait()
    for i in range(ZY):
        wide_ref[i] = near_ref[...]
    store = pltpu.make_async_copy(wide_ref, rows_ref, sems.at[5])
    store.start()
    for copy in copies:
        copy.wait()
    store.wait()


def head_body(
    at_ref, rows_ref, gain_ref, o0, o1, o2, o3, p0, p1, p2, p3, out_ref, weights_ref, near_ref, sem
):
    fetch = pltpu.make_async_copy(gain_ref, near_ref, sem)
    fetch.start()
    x_at = at_ref[0]
    c_at = at_ref[1]
    for shift, (own, other) in enumerate(zip((o0, o1, o2, o3), (p0, p1, p2, p3), strict=True)):
        place = ((x_at - shift) & 3) * 32
        for core, ref in ((c_at, own), (1 - c_at, other)):
            for kind in range(4):
                start = pl.multiple_of(kind * HD + place + core * 16, 16)
                weights_ref[pl.ds(start, 16), :] = ref[kind * 16 : kind * 16 + 16, :]
    scaled = rms_scale(rows_ref[...].astype(F32))
    fetch.wait()
    normed = (scaled * near_ref[...]).astype(BF16)
    out_ref[...] = nt(normed, weights_ref[...]).astype(BF16)


PARTS = 4


def mixer_body(
    joined_ref,
    x_ref,
    decay_ref,
    beta_ref,
    head_gain_ref,
    w_out_ref,
    gain_post_ref,
    gain_ffn_ref,
    send_ref,
    state_ref,
    sent_ref,
    second_ref,
    keys_ref,
    change_ref,
    fade_ref,
    mixed_ref,
    held_ref,
    held_out_ref,
    sems,
):
    held_in, out_in = [], []
    for i in range(PARTS):
        heads = pl.ds(i * (H // PARTS), H // PARTS)
        held_in.append(
            pltpu.make_async_copy(state_ref.at[:, heads], held_ref.at[:, heads], sems.at[i])
        )
        lines = pl.ds(i * (D // PARTS), D // PARTS)
        out_in.append(
            pltpu.make_async_copy(w_out_ref.at[lines], held_out_ref.at[lines], sems.at[PARTS + i])
        )
    for fetch in held_in + out_in:
        fetch.start()
    first = x_ref[...].astype(F32)
    fade = decay_ref[...]
    beta = beta_ref[...]
    turn = iota((4 * SEQ, HD), 0) % SEQ
    for head in range(H):
        if head % (H // PARTS) == 0:
            held_in[head // (H // PARTS)].wait()
        block = joined_ref[head].astype(F32)
        query = silu(block[:, :HD])
        query = query * (
            lax.rsqrt(jnp.sum(query * query, axis=-1, keepdims=True) + EPS) * HD ** (-0.5)
        )
        keys = silu(block[:, HD : 2 * HD])
        keys = keys * lax.rsqrt(jnp.sum(keys * keys, axis=-1, keepdims=True) + EPS)
        values = silu(block[:, 2 * HD : 3 * HD])
        left = jnp.concatenate([*halves(keys), *halves(query)], axis=0)
        both = jnp.zeros((4 * SEQ, HD), F32)
        for row in range(SEQ):
            both = jnp.where(turn == row, mm(left, held_ref[row, head]), both)
        faded = fade[:, head : head + 1]
        guess = faded * (both[:SEQ] + both[SEQ : 2 * SEQ])
        change = beta[:, head : head + 1] * (values - guess)
        output = faded * (both[2 * SEQ : 3 * SEQ] + both[3 * SEQ :])
        output = output + jnp.sum(query * keys, axis=-1, keepdims=True) * change
        output = rms_scale(output) * head_gain_ref[...] * silu(block[:, 3 * HD :])
        mixed_ref[:, head * HD : (head + 1) * HD] = output.astype(BF16)
        spot = slice(head * SEQ, (head + 1) * SEQ)
        keys_ref[spot, :] = keys
        change_ref[spot, :] = change
        fade_ref[spot, :] = jnp.broadcast_to(faded, (SEQ, HD))
    branch = jnp.zeros((SEQ, D), F32)
    for i in range(PARTS):
        out_in[i].wait()
        lines = slice(i * (D // PARTS), (i + 1) * (D // PARTS))
        branch = branch + mm(mixed_ref[:, lines], held_out_ref[lines, :])
    second = first + rms_scale(branch) * gain_post_ref[...]
    second_ref[...] = second
    normed_two = rms_scale(second) * gain_ffn_ref[...]
    runs = jnp.concatenate(
        [normed_two[:, i * RUN : (i + 1) * RUN] for i in range(QUART)], axis=0
    ).astype(BF16)
    sent_ref[...] = mm(send_ref[...], runs).astype(BF16)


HEADS = 2


def state_body(keys_ref, change_ref, fade_ref, state_ref, out_ref):
    for head in range(HEADS):
        spot = slice(head * SEQ, (head + 1) * SEQ)
        tall = keys_ref[spot, :].T
        for row in range(SEQ):
            at = head * SEQ + row
            held = state_ref[row, head].astype(F32) * fade_ref[at : at + 1, :]
            held = held + tall[:, row : row + 1] * change_ref[at : at + 1, :]
            out_ref[row, head] = held.astype(BF16)


def state_call(keys, change, fade, state):
    small = pl.BlockSpec((HEADS * SEQ, HD), lambda i: (i, 0))
    large = pl.BlockSpec((SEQ, HEADS, HD, HD), lambda i: (0, i, 0, 0))
    return pl.pallas_call(
        state_body,
        grid=(H // HEADS,),
        in_specs=[small, small, small, large],
        out_specs=large,
        out_shape=shape(state.shape, BF16),
        name="new_state",
        compiler_params=pltpu.CompilerParams(vmem_limit_bytes=8 * MIB),
        cost_estimate=pl.CostEstimate(flops=40_000_000, bytes_accessed=8 * MIB, transcendentals=0),
    )(keys, change, fade, state)


def expert_body(block_ref, g0, g1, u0, u1, d0, d1, out_ref):
    line = iota((LINES, LINES), 0)
    source = (line % ROWS) * QUART + line // ROWS
    gather = (iota((LINES, LINES), 1) == source).astype(BF16)
    runs = mm(gather, block_ref[...]).astype(BF16)
    rows = jnp.concatenate([runs[i * ROWS : (i + 1) * ROWS] for i in range(QUART)], axis=1)
    part = jnp.zeros((ROWS, D), F32)
    for gate_ref, up_ref, down_ref in ((g0, u0, d0), (g1, u1, d1)):
        hidden = clamped_unit(mm(rows, gate_ref[...]), mm(rows, up_ref[...])).astype(BF16)
        part = part + mm(hidden, down_ref[...])
    part = part.astype(BF16)
    runs = jnp.concatenate([part[:, i * RUN : (i + 1) * RUN] for i in range(QUART)], axis=0)
    back = (iota((LINES, LINES), 1) == (line % QUART) * ROWS + line // QUART).astype(BF16)
    out_ref[...] = mm(back, runs).astype(BF16)


def finish_body(back_ref, mix_ref, second_ref, gain_ref, out_ref):
    runs = mm(mix_ref[...], back_ref[...])
    runs = runs[: QUART * SEQ] + runs[QUART * SEQ :]
    moe = jnp.concatenate([runs[i * SEQ : (i + 1) * SEQ] for i in range(QUART)], axis=1)
    out_ref[...] = (second_ref[...] + rms_scale(moe) * gain_ref[...]).astype(BF16)


def swap_cores(values):
    return lax.ppermute(values, "c", [(0, 1), (1, 0)])


def exchange(values, axes):
    return lax.all_to_all(values, axes, 0, 0, tiled=True)


def shards(
    residual_in,
    gain_mix_pre,
    w_query,
    w_key,
    w_value,
    w_outgate,
    w_decay,
    w_beta,
    decay_scale,
    decay_bias,
    head_gain,
    w_out,
    gain_mix_post,
    state_cache,
    gain_ffn_pre,
    routes,
    route_logits,
    w_gate,
    w_up,
    w_down,
    gain_ffn_post,
):
    at = jnp.stack([lax.axis_index("x"), lax.axis_index("c")]).astype(jnp.int32)
    flat = lambda gain: gain.reshape(1, -1)
    vmem = pl.BlockSpec(memory_space=pltpu.VMEM)
    smem = pl.BlockSpec(memory_space=pltpu.SMEM)
    far = pl.BlockSpec(memory_space=pltpu.HBM)
    hbm = lambda value: pltpu.with_memory_space_constraint(value, pltpu.HBM)
    spread, own = call(
        prepare_body,
        (shape((ZY, SEQ, D), BF16), shape((64, D), BF16)),
        4,
        specs=[far] * 5,
        outs_specs=[far, vmem],
        scratch=[
            pltpu.VMEM((SEQ, D), BF16),
            pltpu.VMEM((ZY, SEQ, D), BF16),
            pltpu.SemaphoreType.DMA((6,)),
        ],
    )(*(hbm(value) for value in (residual_in, w_query.T, w_key.T, w_value.T, w_outgate.T)))
    rows = exchange(spread, ("z", "y"))
    mine = [own] + [
        lax.ppermute(own, "x", [(i, (i + shift) % 4) for i in range(4)]) for shift in (1, 2, 3)
    ]
    other = [swap_cores(one) for one in mine]
    gate_other = swap_cores(w_gate)
    up_other = swap_cores(w_up)
    down_other = swap_cores(w_down)

    columns = call(
        head_body,
        shape((ZY * SEQ, 4 * HD), BF16),
        6,
        scratch=[
            pltpu.VMEM((4 * HD, D), BF16),
            pltpu.VMEM((1, D), F32),
            pltpu.SemaphoreType.DMA,
        ],
        specs=[smem, vmem, far] + [vmem] * 8,
    )(at, rows.reshape(ZY * SEQ, D), hbm(flat(gain_mix_pre)), *mine, *other)
    joined = exchange(columns.reshape(ZY, SEQ, 4 * HD), ("z", "y"))
    send, mix, decay, beta = call(
        route_body,
        (
            shape((LINES, QUART * SEQ), BF16),
            shape((2 * QUART * SEQ, LINES), BF16),
            shape((SEQ, H), F32),
            shape((SEQ, H), F32),
        ),
        8,
    )(
        routes,
        route_logits,
        residual_in,
        flat(gain_mix_pre),
        w_decay.T,
        w_beta.T,
        flat(decay_scale),
        flat(decay_bias),
    )

    small = shape((H * SEQ, HD), F32)
    sent, second, keys, change, fade = call(
        mixer_body,
        (shape((LINES, RUN), BF16), shape((SEQ, D), F32), small, small, small),
        16,
        specs=[vmem] * 5 + [far] + [vmem] * 3 + [far],
        scratch=[
            pltpu.VMEM((SEQ, H * HD), BF16),
            pltpu.VMEM((SEQ, H, HD, HD), BF16),
            pltpu.VMEM((D, D), BF16),
            pltpu.SemaphoreType.DMA((2 * PARTS,)),
        ],
    )(
        joined,
        residual_in,
        decay,
        beta,
        flat(head_gain),
        hbm(w_out),
        flat(gain_mix_post),
        flat(gain_ffn_pre),
        send,
        hbm(state_cache),
    )
    block = exchange(sent.reshape(CHIPS, CAP * QUART, RUN), ("z", "y", "x"))
    new_state = state_call(keys, change, fade, hbm(state_cache))
    part = call(expert_body, shape((LINES, RUN), BF16), 20)(
        block.reshape(LINES, RUN), w_gate, gate_other, w_up, up_other, w_down, down_other
    )
    back = exchange(part.reshape(CHIPS, CAP * QUART, RUN), ("z", "y", "x"))
    result = call(finish_body, shape((SEQ, D), BF16), 8)(
        back.reshape(LINES, RUN), mix, second, flat(gain_ffn_post)
    )
    return (result, new_state)


def solution(mesh):
    torus = Mesh(mesh.devices.reshape(4, 4, 4, 2), ("z", "y", "x", "c"))
    ep = ("z", "y", "x", "c")
    in_specs = (
        P(ep, None),
        P(),
        P(None, ep),
        P(None, ep),
        P(None, ep),
        P(None, ep),
        P(),
        P(),
        P(),
        P(),
        P(),
        P(),
        P(),
        P(ep, None, None, None),
        P(),
        P(ep, None),
        P(ep, None),
        P(None, ep),
        P(None, ep),
        P(ep, None),
        P(),
    )
    out_specs = (P(ep, None), P(ep, None, None, None))
    return jax.shard_map(
        shards, mesh=torus, in_specs=in_specs, out_specs=out_specs, check_vma=False
    )
```

```python
import jax
import jax.numpy as jnp
from jax import lax
from jax.experimental import pallas as pl
from jax.experimental.pallas import tpu as pltpu
from jax.sharding import Mesh
from jax.sharding import PartitionSpec as P


H = 16
HD = 128
D = 2048
TOPK = 4
EXPERTS = 32
CAP = 2
SEQ = 8
ZY = 16
CHIPS = 64
QUART = 4
RUN = D // QUART
LINES = CHIPS * CAP * QUART
ROWS = CHIPS * CAP
PARTS = 4
GROUP = 8
EARLY = 512
LATER = D - EARLY


EPS = 1e-06
LIMIT = 7.0
ALPHA = 1.702

F32 = jnp.float32
BF16 = jnp.bfloat16
MIB = 1 << 20


def iota(shape, dimension):
    return lax.broadcasted_iota(jnp.int32, shape, dimension)


def nt(left, right):
    return lax.dot_general(left, right, (((1,), (1,)), ((), ())), preferred_element_type=F32)


def mm(left, right):
    return jnp.dot(left, right, preferred_element_type=F32)


def silu(values):
    return values * jax.nn.sigmoid(values)


def rms_scale(values):
    return values * lax.rsqrt(jnp.mean(values * values, axis=-1, keepdims=True) + EPS)


def halves(values):
    high = values.astype(BF16)
    return high, (values - high.astype(F32)).astype(BF16)


def clamped_unit(gate, upper):
    glu = jnp.minimum(gate, LIMIT)
    linear = jnp.clip(upper, -LIMIT, LIMIT)
    return glu * jax.nn.sigmoid(ALPHA * glu) * (linear + 1.0)


def call(body, outs, limit, scratch=(), specs=None, outs_specs=None, flops=0):
    return pl.pallas_call(
        body,
        out_shape=outs,
        **({} if specs is None else {"in_specs": specs}),
        **({} if outs_specs is None else {"out_specs": outs_specs}),
        scratch_shapes=list(scratch),
        compiler_params=pltpu.CompilerParams(vmem_limit_bytes=limit * MIB),
        cost_estimate=pl.CostEstimate(flops=flops, bytes_accessed=0, transcendentals=0),
    )


def shape(dims, dtype):
    return jax.ShapeDtypeStruct(dims, dtype)


def route_body(*refs):
    far, (send_ref, mix_ref, fade_ref, beta_ref), near = refs[:8], refs[8:12], refs[12:20]
    copies = [
        pltpu.make_async_copy(one, ref, refs[20].at[i])
        for i, (one, ref) in enumerate(zip(far, near, strict=True))
    ]
    for copy in copies:
        copy.start()
    for copy in copies:
        copy.wait()
    (
        routes_ref,
        logits_ref,
        x_ref,
        gain_pre_ref,
        decay_w_ref,
        beta_w_ref,
        scale_ref,
        bias_ref,
    ) = near
    normed = (rms_scale(x_ref[...].astype(F32)) * gain_pre_ref[...]).astype(BF16)
    raised = nt(normed, decay_w_ref[...]) + bias_ref[...]
    soft = jnp.maximum(raised, 0.0) + jnp.log1p(jnp.exp(-jnp.abs(raised)))
    fade = jnp.exp(-scale_ref[...] * soft)
    beta = jax.nn.sigmoid(nt(normed, beta_w_ref[...]))
    for head in range(H):
        fade_ref[head] = jnp.broadcast_to(fade[:, head : head + 1], (SEQ, HD))
        beta_ref[head] = jnp.broadcast_to(beta[:, head : head + 1], (SEQ, HD))
    routes = routes_ref[...].astype(F32).T
    raised = jnp.exp(logits_ref[...].T)
    weights = raised / jnp.sum(raised, axis=-1, keepdims=True)
    named = iota((SEQ, EXPERTS), 1)
    hits = jnp.zeros((SEQ, EXPERTS), F32)
    weighed = jnp.zeros((SEQ, EXPERTS), F32)
    for j in range(TOPK):
        hit = (routes[:, j : j + 1] == named.astype(F32)).astype(F32)
        hits = hits + hit
        weighed = weighed + hit * weights[:, j : j + 1]
    earlier = (iota((SEQ, SEQ), 0) > iota((SEQ, SEQ), 1)).astype(BF16)
    slots = mm(earlier, hits.astype(BF16))
    line = iota((LINES, EXPERTS), 0)
    expert_of = (line // (2 * CAP * QUART)) == iota((LINES, EXPERTS), 1)
    slot_of = (line // QUART) % CAP
    column = iota((LINES, QUART * SEQ), 1)
    same_run = (iota((LINES, QUART * SEQ), 0) % QUART) == (column // SEQ)
    send = jnp.zeros((LINES, QUART * SEQ), F32)
    mix = jnp.zeros((LINES, QUART * SEQ), F32)
    for slot in range(CAP):
        chosen = (expert_of & (slot_of == slot)).astype(BF16)
        here = slots == slot
        picks = jnp.where(here, hits, 0.0)
        shares = jnp.where(here, weighed, 0.0)
        high, low = halves(jnp.concatenate([shares] * QUART, axis=0))
        send = send + nt(chosen, jnp.concatenate([picks] * QUART, axis=0).astype(BF16))
        mix = mix + (nt(chosen, high) + nt(chosen, low))
    send_ref[...] = jnp.where(same_run, send, 0.0).astype(BF16)
    high, low = halves(jnp.where(same_run, mix, 0.0).T)
    mix_ref[...] = jnp.concatenate([high, low], axis=0)


def prepare_body(x_ref, q_ref, k_ref, v_ref, z_ref, rows_ref, own_ref, near_ref, wide_ref, sems):
    fetch = pltpu.make_async_copy(x_ref, near_ref, sems.at[4])
    fetch.start()
    copies = [
        pltpu.make_async_copy(ref, own_ref.at[pl.ds(i * 16, 16)], sems.at[i])
        for i, ref in enumerate((q_ref, k_ref, v_ref, z_ref))
    ]
    for copy in copies:
        copy.start()
    fetch.wait()
    for i in range(ZY):
        wide_ref[i] = near_ref[...]
    store = pltpu.make_async_copy(wide_ref, rows_ref, sems.at[5])
    store.start()
    for copy in copies:
        copy.wait()
    store.wait()


def head_body(
    rows_ref,
    gain_ref,
    state_ref,
    w_out_ref,
    o0,
    o1,
    o2,
    o3,
    p0,
    p1,
    p2,
    p3,
    out_ref,
    held_ref,
    w_near_ref,
    weights_ref,
    near_ref,
    sems,
):
    fetch = pltpu.make_async_copy(gain_ref, near_ref, sems.at[SEQ + 1])
    fetch.start()
    later = [
        pltpu.make_async_copy(state_ref.at[row], held_ref.at[row], sems.at[row])
        for row in range(SEQ)
    ]
    later.append(pltpu.make_async_copy(w_out_ref.at[pl.ds(0, EARLY)], w_near_ref, sems.at[SEQ]))
    for copy in later:
        copy.start()
    x_at = lax.axis_index("x")
    c_at = lax.axis_index("c")
    for shift, (own, other) in enumerate(zip((o0, o1, o2, o3), (p0, p1, p2, p3), strict=True)):
        place = ((x_at - shift) & 3) * 32
        for core, ref in ((c_at, own), (1 - c_at, other)):
            for kind in range(4):
                start = pl.multiple_of(kind * HD + place + core * 16, 16)
                weights_ref[pl.ds(start, 16), :] = ref[kind * 16 : kind * 16 + 16, :]
    scaled = rms_scale(rows_ref[...].astype(F32))
    fetch.wait()
    normed = (scaled * near_ref[...]).astype(BF16)
    out_ref[...] = nt(normed, weights_ref[...]).astype(BF16)
    for copy in later:
        copy.wait()


def mixer_body(
    joined_ref,
    x_ref,
    fade_ref,
    beta_ref,
    head_gain_ref,
    w_out_ref,
    gain_post_ref,
    gain_ffn_ref,
    send_ref,
    state_ref,
    w_last_ref,
    sent_ref,
    second_ref,
    keys_ref,
    change_ref,
    mixed_ref,
    last_ref,
    sems,
):
    out_in = []
    for i in range(PARTS):
        lines = pl.ds(i * (LATER // PARTS), LATER // PARTS)
        out_in.append(
            pltpu.make_async_copy(
                w_last_ref.at[pl.ds(EARLY + i * (LATER // PARTS), LATER // PARTS)],
                last_ref.at[lines],
                sems.at[i],
            )
        )
    for fetch in out_in:
        fetch.start()
    turn = iota((4 * SEQ, HD), 0) % SEQ

    def one_head(head):
        block = joined_ref[head].astype(F32)
        query = silu(block[:, :HD])
        query = query * (
            lax.rsqrt(jnp.sum(query * query, axis=-1, keepdims=True) + EPS) * HD ** (-0.5)
        )
        keys = silu(block[:, HD : 2 * HD])
        keys = keys * lax.rsqrt(jnp.sum(keys * keys, axis=-1, keepdims=True) + EPS)
        values = silu(block[:, 2 * HD : 3 * HD])
        left = jnp.concatenate([*halves(keys), *halves(query)], axis=0)
        both = mm(left, state_ref[0, head])
        for row in range(1, SEQ):
            both = jnp.where(turn == row, mm(left, state_ref[row, head]), both)
        faded = fade_ref[head]
        guess = faded * (both[:SEQ] + both[SEQ : 2 * SEQ])
        change = beta_ref[head] * (values - guess)
        output = faded * (both[2 * SEQ : 3 * SEQ] + both[3 * SEQ :])
        output = output + jnp.sum(query * keys, axis=-1, keepdims=True) * change
        output = rms_scale(output) * head_gain_ref[...] * silu(block[:, 3 * HD :])
        mixed_ref[head] = output
        keys_ref[head] = keys
        change_ref[head] = change

    def some_heads(step, carry):
        for i in range(GROUP):
            one_head(step * GROUP + i)
        return carry

    lax.fori_loop(0, H // GROUP, some_heads, 0)
    mixed = jnp.concatenate([mixed_ref[head] for head in range(H)], axis=1).astype(BF16)
    first = x_ref[...].astype(F32)
    branch = mm(mixed[:, :EARLY], w_out_ref[...])
    for i in range(PARTS):
        out_in[i].wait()
        lines = slice(i * (LATER // PARTS), (i + 1) * (LATER // PARTS))
        here = slice(EARLY + i * (LATER // PARTS), EARLY + (i + 1) * (LATER // PARTS))
        branch = branch + mm(mixed[:, here], last_ref[lines, :])
    second = first + rms_scale(branch) * gain_post_ref[...]
    second_ref[...] = second
    normed_two = rms_scale(second) * gain_ffn_ref[...]
    runs = jnp.concatenate(
        [normed_two[:, i * RUN : (i + 1) * RUN] for i in range(QUART)], axis=0
    ).astype(BF16)
    sent_ref[...] = mm(send_ref[...], runs).astype(BF16)


HEADS = 2


def state_body(keys_ref, change_ref, fade_ref, state_ref, out_ref):
    for head in range(HEADS):
        tall = keys_ref[head].T
        for row in range(SEQ):
            held = state_ref[row, head].astype(F32) * fade_ref[head, row : row + 1, :]
            held = held + tall[:, row : row + 1] * change_ref[head, row : row + 1, :]
            out_ref[row, head] = held.astype(BF16)


def state_call(keys, change, fade, state):
    small = pl.BlockSpec((HEADS, SEQ, HD), lambda i: (i, 0, 0))
    large = pl.BlockSpec((SEQ, HEADS, HD, HD), lambda i: (0, i, 0, 0))
    return pl.pallas_call(
        state_body,
        grid=(H // HEADS,),
        in_specs=[small, small, small, large],
        out_specs=large,
        out_shape=shape(state.shape, BF16),
        name="new_state",
        compiler_params=pltpu.CompilerParams(vmem_limit_bytes=8 * MIB),
        cost_estimate=pl.CostEstimate(flops=40_000_000, bytes_accessed=8 * MIB, transcendentals=0),
    )(keys, change, fade, state)


def expert_body(block_ref, g0, g1, u0, u1, d0, d1, out_ref):
    line = iota((LINES, LINES), 0)
    source = (line % ROWS) * QUART + line // ROWS
    gather = (iota((LINES, LINES), 1) == source).astype(BF16)
    runs = mm(gather, block_ref[...]).astype(BF16)
    rows = jnp.concatenate([runs[i * ROWS : (i + 1) * ROWS] for i in range(QUART)], axis=1)
    part = jnp.zeros((ROWS, D), F32)
    for gate_ref, up_ref, down_ref in ((g0, u0, d0), (g1, u1, d1)):
        hidden = clamped_unit(mm(rows, gate_ref[...]), mm(rows, up_ref[...])).astype(BF16)
        part = part + mm(hidden, down_ref[...])
    part = part.astype(BF16)
    runs = jnp.concatenate([part[:, i * RUN : (i + 1) * RUN] for i in range(QUART)], axis=0)
    back = (iota((LINES, LINES), 1) == (line % QUART) * ROWS + line // QUART).astype(BF16)
    out_ref[...] = mm(back, runs).astype(BF16)


def finish_body(back_ref, mix_ref, second_ref, gain_ref, out_ref):
    runs = mm(mix_ref[...], back_ref[...])
    runs = runs[: QUART * SEQ] + runs[QUART * SEQ :]
    moe = jnp.concatenate([runs[i * SEQ : (i + 1) * SEQ] for i in range(QUART)], axis=1)
    out_ref[...] = (second_ref[...] + rms_scale(moe) * gain_ref[...]).astype(BF16)


def swap_cores(values):
    return lax.ppermute(values, "c", [(0, 1), (1, 0)])


def exchange(values, axes):
    return lax.all_to_all(values, axes, 0, 0, tiled=True)


def shards(
    residual_in,
    gain_mix_pre,
    w_query,
    w_key,
    w_value,
    w_outgate,
    w_decay,
    w_beta,
    decay_scale,
    decay_bias,
    head_gain,
    w_out,
    gain_mix_post,
    state_cache,
    gain_ffn_pre,
    routes,
    route_logits,
    w_gate,
    w_up,
    w_down,
    gain_ffn_post,
):
    flat = lambda gain: gain.reshape(1, -1)
    vmem = pl.BlockSpec(memory_space=pltpu.VMEM)
    far = pl.BlockSpec(memory_space=pltpu.HBM)
    hbm = lambda value: pltpu.with_memory_space_constraint(value, pltpu.HBM)
    spread, own = call(
        prepare_body,
        (shape((ZY, SEQ, D), BF16), shape((64, D), BF16)),
        4,
        specs=[far] * 5,
        outs_specs=[far, vmem],
        scratch=[
            pltpu.VMEM((SEQ, D), BF16),
            pltpu.VMEM((ZY, SEQ, D), BF16),
            pltpu.SemaphoreType.DMA((6,)),
        ],
    )(*(hbm(value) for value in (residual_in, w_query.T, w_key.T, w_value.T, w_outgate.T)))
    rows = exchange(spread, ("z", "y"))
    mine = [own] + [
        lax.ppermute(own, "x", [(i, (i + shift) % 4) for i in range(4)]) for shift in (1, 2, 3)
    ]
    other = [swap_cores(one) for one in mine]
    gate_other = swap_cores(w_gate)
    up_other = swap_cores(w_up)
    down_other = swap_cores(w_down)

    columns, held, w_near = call(
        head_body,
        (
            shape((ZY * SEQ, 4 * HD), BF16),
            shape(state_cache.shape, BF16),
            shape((EARLY, D), BF16),
        ),
        6,
        scratch=[
            pltpu.VMEM((4 * HD, D), BF16),
            pltpu.VMEM((1, D), F32),
            pltpu.SemaphoreType.DMA((SEQ + 2,)),
        ],
        specs=[vmem, far, far, far] + [vmem] * 8,
    )(
        rows.reshape(ZY * SEQ, D),
        hbm(flat(gain_mix_pre)),
        hbm(state_cache),
        hbm(w_out),
        *mine,
        *other,
    )
    joined = exchange(columns.reshape(ZY, SEQ, 4 * HD), ("z", "y"))
    wanted = (
        routes.T,
        route_logits.T,
        residual_in,
        flat(gain_mix_pre),
        w_decay.T,
        w_beta.T,
        flat(decay_scale),
        flat(decay_bias),
    )
    send, mix, decay, beta = call(
        route_body,
        (
            shape((LINES, QUART * SEQ), BF16),
            shape((2 * QUART * SEQ, LINES), BF16),
            shape((H, SEQ, HD), F32),
            shape((H, SEQ, HD), F32),
        ),
        4,
        specs=[far] * 8,
        scratch=[pltpu.VMEM(value.shape, value.dtype) for value in wanted]
        + [pltpu.SemaphoreType.DMA((8,))],
    )(*(hbm(value) for value in wanted))

    small = shape((H, SEQ, HD), F32)
    sent, second, keys, change = call(
        mixer_body,
        (shape((LINES, RUN), BF16), shape((SEQ, D), F32), small, small),
        12,
        specs=[vmem] * 10 + [far],
        scratch=[
            pltpu.VMEM((H, SEQ, HD), F32),
            pltpu.VMEM((LATER, D), BF16),
            pltpu.SemaphoreType.DMA((PARTS,)),
        ],
    )(
        joined,
        residual_in,
        decay,
        beta,
        flat(head_gain),
        w_near,
        flat(gain_mix_post),
        flat(gain_ffn_pre),
        send,
        held,
        hbm(w_out),
    )
    block = exchange(sent.reshape(CHIPS, CAP * QUART, RUN), ("z", "y", "x"))
    new_state = state_call(keys, change, decay, hbm(state_cache))
    part = call(expert_body, shape((LINES, RUN), BF16), 16)(
        block.reshape(LINES, RUN), w_gate, gate_other, w_up, up_other, w_down, down_other
    )
    back = exchange(part.reshape(CHIPS, CAP * QUART, RUN), ("z", "y", "x"))
    result = call(finish_body, shape((SEQ, D), BF16), 8)(
        back.reshape(LINES, RUN), mix, second, flat(gain_ffn_post)
    )
    return (result, new_state)


def solution(mesh):
    torus = Mesh(mesh.devices.reshape(4, 4, 4, 2), ("z", "y", "x", "c"))
    ep = ("z", "y", "x", "c")
    in_specs = (
        P(ep, None),
        P(),
        P(None, ep),
        P(None, ep),
        P(None, ep),
        P(None, ep),
        P(),
        P(),
        P(),
        P(),
        P(),
        P(),
        P(),
        P(ep, None, None, None),
        P(),
        P(ep, None),
        P(ep, None),
        P(None, ep),
        P(None, ep),
        P(ep, None),
        P(),
    )
    out_specs = (P(ep, None), P(ep, None, None, None))
    return jax.shard_map(
        shards, mesh=torus, in_specs=in_specs, out_specs=out_specs, check_vma=False
    )
```

```python
import jax
import jax.numpy as jnp
from jax import lax
from jax.experimental import pallas as pl
from jax.experimental.pallas import tpu as pltpu
from jax.sharding import Mesh
from jax.sharding import PartitionSpec as P


H = 16
HD = 128
D = 2048
TOPK = 4
EXPERTS = 32
CAP = 2
SEQ = 8
ZY = 16
CHIPS = 64
QUART = 4
RUN = D // QUART
LINES = CHIPS * CAP * QUART
ROWS = CHIPS * CAP
PARTS = 7
GROUP = 8
EARLY = 256
LATER = D - EARLY


EPS = 1e-06
LIMIT = 7.0
ALPHA = 1.702

F32 = jnp.float32
BF16 = jnp.bfloat16
MIB = 1 << 20


def iota(shape, dimension):
    return lax.broadcasted_iota(jnp.int32, shape, dimension)


def nt(left, right):
    return lax.dot_general(left, right, (((1,), (1,)), ((), ())), preferred_element_type=F32)


def mm(left, right):
    return jnp.dot(left, right, preferred_element_type=F32)


def silu(values):
    return values * jax.nn.sigmoid(values)


def rms_scale(values):
    return values * lax.rsqrt(jnp.mean(values * values, axis=-1, keepdims=True) + EPS)


def halves(values):
    high = values.astype(BF16)
    return high, (values - high.astype(F32)).astype(BF16)


def clamped_unit(gate, upper):
    glu = jnp.minimum(gate, LIMIT)
    linear = jnp.clip(upper, -LIMIT, LIMIT)
    return glu * jax.nn.sigmoid(ALPHA * glu) * (linear + 1.0)


def call(body, outs, limit, scratch=(), specs=None, outs_specs=None, flops=0):
    return pl.pallas_call(
        body,
        out_shape=outs,
        **({} if specs is None else {"in_specs": specs}),
        **({} if outs_specs is None else {"out_specs": outs_specs}),
        scratch_shapes=list(scratch),
        compiler_params=pltpu.CompilerParams(vmem_limit_bytes=limit * MIB),
        cost_estimate=pl.CostEstimate(flops=flops, bytes_accessed=0, transcendentals=0),
    )


def shape(dims, dtype):
    return jax.ShapeDtypeStruct(dims, dtype)


def route_body(*refs):
    far, (send_ref, mix_ref, fade_ref, beta_ref), near = refs[:8], refs[8:12], refs[12:20]
    copies = [
        pltpu.make_async_copy(one, ref, refs[20].at[i])
        for i, (one, ref) in enumerate(zip(far, near, strict=True))
    ]
    for copy in copies:
        copy.start()
    for copy in copies:
        copy.wait()
    (
        routes_ref,
        logits_ref,
        x_ref,
        gain_pre_ref,
        decay_w_ref,
        beta_w_ref,
        scale_ref,
        bias_ref,
    ) = near
    normed = (rms_scale(x_ref[...].astype(F32)) * gain_pre_ref[...]).astype(BF16)
    raised = nt(normed, decay_w_ref[...]) + bias_ref[...]
    soft = jnp.maximum(raised, 0.0) + jnp.log1p(jnp.exp(-jnp.abs(raised)))
    fade = jnp.exp(-scale_ref[...] * soft)
    beta = jax.nn.sigmoid(nt(normed, beta_w_ref[...]))
    for head in range(H):
        fade_ref[head] = jnp.broadcast_to(fade[:, head : head + 1], (SEQ, HD))
        beta_ref[head] = jnp.broadcast_to(beta[:, head : head + 1], (SEQ, HD))
    routes = routes_ref[...].astype(F32).T
    raised = jnp.exp(logits_ref[...].T)
    weights = raised / jnp.sum(raised, axis=-1, keepdims=True)
    named = iota((SEQ, EXPERTS), 1)
    hits = jnp.zeros((SEQ, EXPERTS), F32)
    weighed = jnp.zeros((SEQ, EXPERTS), F32)
    for j in range(TOPK):
        hit = (routes[:, j : j + 1] == named.astype(F32)).astype(F32)
        hits = hits + hit
        weighed = weighed + hit * weights[:, j : j + 1]
    earlier = (iota((SEQ, SEQ), 0) > iota((SEQ, SEQ), 1)).astype(BF16)
    slots = mm(earlier, hits.astype(BF16))
    line = iota((LINES, EXPERTS), 0)
    expert_of = (line // (2 * CAP * QUART)) == iota((LINES, EXPERTS), 1)
    slot_of = (line // QUART) % CAP
    column = iota((LINES, QUART * SEQ), 1)
    same_run = (iota((LINES, QUART * SEQ), 0) % QUART) == (column // SEQ)
    send = jnp.zeros((LINES, QUART * SEQ), F32)
    mix = jnp.zeros((LINES, QUART * SEQ), F32)
    for slot in range(CAP):
        chosen = (expert_of & (slot_of == slot)).astype(BF16)
        here = slots == slot
        picks = jnp.where(here, hits, 0.0)
        shares = jnp.where(here, weighed, 0.0)
        high, low = halves(jnp.concatenate([shares] * QUART, axis=0))
        send = send + nt(chosen, jnp.concatenate([picks] * QUART, axis=0).astype(BF16))
        mix = mix + (nt(chosen, high) + nt(chosen, low))
    send_ref[...] = jnp.where(same_run, send, 0.0).astype(BF16)
    high, low = halves(jnp.where(same_run, mix, 0.0).T)
    mix_ref[...] = jnp.concatenate([high, low], axis=0)


def prepare_body(x_ref, q_ref, k_ref, v_ref, z_ref, rows_ref, own_ref, near_ref, wide_ref, sems):
    fetch = pltpu.make_async_copy(x_ref, near_ref, sems.at[4])
    fetch.start()
    copies = [
        pltpu.make_async_copy(ref, own_ref.at[pl.ds(i * 16, 16)], sems.at[i])
        for i, ref in enumerate((q_ref, k_ref, v_ref, z_ref))
    ]
    for copy in copies:
        copy.start()
    fetch.wait()
    for i in range(ZY):
        wide_ref[i] = near_ref[...]
    store = pltpu.make_async_copy(wide_ref, rows_ref, sems.at[5])
    store.start()
    for copy in copies:
        copy.wait()
    store.wait()


def head_body(
    rows_ref,
    gain_ref,
    state_ref,
    w_out_ref,
    o0,
    o1,
    o2,
    o3,
    p0,
    p1,
    p2,
    p3,
    out_ref,
    held_ref,
    w_near_ref,
    weights_ref,
    near_ref,
    ready_ref,
    sems,
):
    fetch = pltpu.make_async_copy(gain_ref, near_ref, sems.at[SEQ + 1])
    fetch.start()
    later = [
        pltpu.make_async_copy(state_ref.at[row], held_ref.at[row], sems.at[row])
        for row in range(SEQ)
    ]
    later.append(pltpu.make_async_copy(w_out_ref.at[pl.ds(0, EARLY)], w_near_ref, sems.at[SEQ]))
    for copy in later:
        copy.start()
    x_at = lax.axis_index("x")
    c_at = lax.axis_index("c")
    for shift, (own, other) in enumerate(zip((o0, o1, o2, o3), (p0, p1, p2, p3), strict=True)):
        place = ((x_at - shift) & 3) * 32
        for core, ref in ((c_at, own), (1 - c_at, other)):
            for kind in range(4):
                start = pl.multiple_of(kind * HD + place + core * 16, 16)
                weights_ref[pl.ds(start, 16), :] = ref[kind * 16 : kind * 16 + 16, :]
    scaled = rms_scale(rows_ref[...].astype(F32))
    fetch.wait()
    normed = (scaled * near_ref[...]).astype(BF16)
    ready_ref[...] = normed

    def one_kind(kind, carry):
        lines = pl.ds(pl.multiple_of(kind * 2 * HD, 2 * HD), 2 * HD)
        out_ref[:, lines] = nt(ready_ref[...], weights_ref[lines, :]).astype(BF16)
        return carry

    lax.fori_loop(0, 2, one_kind, 0)
    for copy in later:
        copy.wait()


def mixer_body(
    joined_ref,
    x_ref,
    fade_ref,
    beta_ref,
    head_gain_ref,
    w_out_ref,
    gain_post_ref,
    gain_ffn_ref,
    send_ref,
    state_ref,
    w_last_ref,
    sent_ref,
    second_ref,
    keys_ref,
    change_ref,
    mixed_ref,
    last_ref,
    sems,
):
    out_in = []
    for i in range(PARTS):
        lines = pl.ds(i * (LATER // PARTS), LATER // PARTS)
        out_in.append(
            pltpu.make_async_copy(
                w_last_ref.at[pl.ds(EARLY + i * (LATER // PARTS), LATER // PARTS)],
                last_ref.at[lines],
                sems.at[i],
            )
        )
    for fetch in out_in:
        fetch.start()
    turn = iota((4 * SEQ, HD), 0) % SEQ

    def one_head(head):
        block = joined_ref[head].astype(F32)
        query = silu(block[:, :HD])
        query = query * (
            lax.rsqrt(jnp.sum(query * query, axis=-1, keepdims=True) + EPS) * HD ** (-0.5)
        )
        keys = silu(block[:, HD : 2 * HD])
        keys = keys * lax.rsqrt(jnp.sum(keys * keys, axis=-1, keepdims=True) + EPS)
        values = silu(block[:, 2 * HD : 3 * HD])
        left = jnp.concatenate([*halves(keys), *halves(query)], axis=0)
        both = mm(left, state_ref[0, head])
        for row in range(1, SEQ):
            both = jnp.where(turn == row, mm(left, state_ref[row, head]), both)
        faded = fade_ref[head]
        guess = faded * (both[:SEQ] + both[SEQ : 2 * SEQ])
        change = beta_ref[head] * (values - guess)
        output = faded * (both[2 * SEQ : 3 * SEQ] + both[3 * SEQ :])
        output = output + jnp.sum(query * keys, axis=-1, keepdims=True) * change
        output = rms_scale(output) * head_gain_ref[...] * silu(block[:, 3 * HD :])
        mixed_ref[head] = output
        keys_ref[head] = keys
        change_ref[head] = change

    def some_heads(step, carry):
        for i in range(GROUP):
            one_head(step * GROUP + i)
        return carry

    lax.fori_loop(0, H // GROUP, some_heads, 0)
    mixed = jnp.concatenate([mixed_ref[head] for head in range(H)], axis=1).astype(BF16)
    first = x_ref[...].astype(F32)
    branch = mm(mixed[:, :EARLY], w_out_ref[...])
    for i in range(PARTS):
        out_in[i].wait()
        lines = slice(i * (LATER // PARTS), (i + 1) * (LATER // PARTS))
        here = slice(EARLY + i * (LATER // PARTS), EARLY + (i + 1) * (LATER // PARTS))
        branch = branch + mm(mixed[:, here], last_ref[lines, :])
    second = first + rms_scale(branch) * gain_post_ref[...]
    second_ref[...] = second
    normed_two = rms_scale(second) * gain_ffn_ref[...]
    runs = jnp.concatenate(
        [normed_two[:, i * RUN : (i + 1) * RUN] for i in range(QUART)], axis=0
    ).astype(BF16)
    sent_ref[...] = mm(send_ref[...], runs).astype(BF16)


HEADS = 2


def state_body(keys_ref, change_ref, fade_ref, state_ref, out_ref):
    for head in range(HEADS):
        tall = keys_ref[head].T
        for row in range(SEQ):
            held = state_ref[row, head].astype(F32) * fade_ref[head, row : row + 1, :]
            held = held + tall[:, row : row + 1] * change_ref[head, row : row + 1, :]
            out_ref[row, head] = held.astype(BF16)


def state_call(keys, change, fade, state):
    small = pl.BlockSpec((HEADS, SEQ, HD), lambda i: (i, 0, 0))
    large = pl.BlockSpec((SEQ, HEADS, HD, HD), lambda i: (0, i, 0, 0))
    return pl.pallas_call(
        state_body,
        grid=(H // HEADS,),
        in_specs=[small, small, small, large],
        out_specs=large,
        out_shape=shape(state.shape, BF16),
        name="new_state",
        compiler_params=pltpu.CompilerParams(vmem_limit_bytes=8 * MIB),
        cost_estimate=pl.CostEstimate(flops=40_000_000, bytes_accessed=8 * MIB, transcendentals=0),
    )(keys, change, fade, state)


def expert_body(block_ref, g0, g1, u0, u1, d0, d1, out_ref):
    line = iota((LINES, LINES), 0)
    source = (line % ROWS) * QUART + line // ROWS
    gather = (iota((LINES, LINES), 1) == source).astype(BF16)
    runs = mm(gather, block_ref[...]).astype(BF16)
    rows = jnp.concatenate([runs[i * ROWS : (i + 1) * ROWS] for i in range(QUART)], axis=1)
    part = jnp.zeros((ROWS, D), F32)
    for gate_ref, up_ref, down_ref in ((g0, u0, d0), (g1, u1, d1)):
        hidden = clamped_unit(mm(rows, gate_ref[...]), mm(rows, up_ref[...])).astype(BF16)
        part = part + mm(hidden, down_ref[...])
    part = part.astype(BF16)
    runs = jnp.concatenate([part[:, i * RUN : (i + 1) * RUN] for i in range(QUART)], axis=0)
    back = (iota((LINES, LINES), 1) == (line % QUART) * ROWS + line // QUART).astype(BF16)
    out_ref[...] = mm(back, runs).astype(BF16)


def finish_body(back_ref, mix_ref, second_ref, gain_ref, out_ref):
    runs = mm(mix_ref[...], back_ref[...])
    runs = runs[: QUART * SEQ] + runs[QUART * SEQ :]
    moe = jnp.concatenate([runs[i * SEQ : (i + 1) * SEQ] for i in range(QUART)], axis=1)
    out_ref[...] = (second_ref[...] + rms_scale(moe) * gain_ref[...]).astype(BF16)


def swap_cores(values):
    return lax.ppermute(values, "c", [(0, 1), (1, 0)])


def exchange(values, axes):
    return lax.all_to_all(values, axes, 0, 0, tiled=True)


def shards(
    residual_in,
    gain_mix_pre,
    w_query,
    w_key,
    w_value,
    w_outgate,
    w_decay,
    w_beta,
    decay_scale,
    decay_bias,
    head_gain,
    w_out,
    gain_mix_post,
    state_cache,
    gain_ffn_pre,
    routes,
    route_logits,
    w_gate,
    w_up,
    w_down,
    gain_ffn_post,
):
    flat = lambda gain: gain.reshape(1, -1)
    vmem = pl.BlockSpec(memory_space=pltpu.VMEM)
    far = pl.BlockSpec(memory_space=pltpu.HBM)
    hbm = lambda value: pltpu.with_memory_space_constraint(value, pltpu.HBM)
    spread, own = call(
        prepare_body,
        (shape((ZY, SEQ, D), BF16), shape((64, D), BF16)),
        4,
        specs=[far] * 5,
        outs_specs=[far, vmem],
        scratch=[
            pltpu.VMEM((SEQ, D), BF16),
            pltpu.VMEM((ZY, SEQ, D), BF16),
            pltpu.SemaphoreType.DMA((6,)),
        ],
    )(*(hbm(value) for value in (residual_in, w_query.T, w_key.T, w_value.T, w_outgate.T)))
    rows = exchange(spread, ("z", "y"))
    mine = [own] + [
        lax.ppermute(own, "x", [(i, (i + shift) % 4) for i in range(4)]) for shift in (1, 2, 3)
    ]
    other = [swap_cores(one) for one in mine]
    gate_other = swap_cores(w_gate)
    up_other = swap_cores(w_up)
    down_other = swap_cores(w_down)

    columns, held, w_near = call(
        head_body,
        (
            shape((ZY * SEQ, 4 * HD), BF16),
            shape(state_cache.shape, BF16),
            shape((EARLY, D), BF16),
        ),
        6,
        scratch=[
            pltpu.VMEM((4 * HD, D), BF16),
            pltpu.VMEM((1, D), F32),
            pltpu.VMEM((ZY * SEQ, D), BF16),
            pltpu.SemaphoreType.DMA((SEQ + 2,)),
        ],
        specs=[vmem, far, far, far] + [vmem] * 8,
    )(
        rows.reshape(ZY * SEQ, D),
        hbm(flat(gain_mix_pre)),
        hbm(state_cache),
        hbm(w_out),
        *mine,
        *other,
    )
    joined = exchange(columns.reshape(ZY, SEQ, 4 * HD), ("z", "y"))
    wanted = (
        routes.T,
        route_logits.T,
        residual_in,
        flat(gain_mix_pre),
        w_decay.T,
        w_beta.T,
        flat(decay_scale),
        flat(decay_bias),
    )
    send, mix, decay, beta = call(
        route_body,
        (
            shape((LINES, QUART * SEQ), BF16),
            shape((2 * QUART * SEQ, LINES), BF16),
            shape((H, SEQ, HD), F32),
            shape((H, SEQ, HD), F32),
        ),
        4,
        specs=[far] * 8,
        scratch=[pltpu.VMEM(value.shape, value.dtype) for value in wanted]
        + [pltpu.SemaphoreType.DMA((8,))],
    )(*(hbm(value) for value in wanted))

    small = shape((H, SEQ, HD), F32)
    sent, second, keys, change = call(
        mixer_body,
        (shape((LINES, RUN), BF16), shape((SEQ, D), F32), small, small),
        12,
        specs=[vmem] * 10 + [far],
        scratch=[
            pltpu.VMEM((H, SEQ, HD), F32),
            pltpu.VMEM((LATER, D), BF16),
            pltpu.SemaphoreType.DMA((PARTS,)),
        ],
    )(
        joined,
        residual_in,
        decay,
        beta,
        flat(head_gain),
        w_near,
        flat(gain_mix_post),
        flat(gain_ffn_pre),
        send,
        held,
        hbm(w_out),
    )
    block = exchange(sent.reshape(CHIPS, CAP * QUART, RUN), ("z", "y", "x"))
    new_state = state_call(keys, change, decay, hbm(state_cache))
    part = call(expert_body, shape((LINES, RUN), BF16), 16)(
        block.reshape(LINES, RUN), w_gate, gate_other, w_up, up_other, w_down, down_other
    )
    back = exchange(part.reshape(CHIPS, CAP * QUART, RUN), ("z", "y", "x"))
    result = call(finish_body, shape((SEQ, D), BF16), 8)(
        back.reshape(LINES, RUN), mix, second, flat(gain_ffn_post)
    )
    return (result, new_state)


def solution(mesh):
    torus = Mesh(mesh.devices.reshape(4, 4, 4, 2), ("z", "y", "x", "c"))
    ep = ("z", "y", "x", "c")
    in_specs = (
        P(ep, None),
        P(),
        P(None, ep),
        P(None, ep),
        P(None, ep),
        P(None, ep),
        P(),
        P(),
        P(),
        P(),
        P(),
        P(),
        P(),
        P(ep, None, None, None),
        P(),
        P(ep, None),
        P(ep, None),
        P(None, ep),
        P(None, ep),
        P(ep, None),
        P(),
    )
    out_specs = (P(ep, None), P(ep, None, None, None))
    return jax.shard_map(
        shards, mesh=torus, in_specs=in_specs, out_specs=out_specs, check_vma=False
    )
```
